32 devices in a mesh: gr: 2 (over x), fs: 8 (over z, y), tp: 2 (over core).
Axes of the slice: x: 2, y: 2, z: 4, core: 2. Of those that a mesh axis runs over, the one named last changes fastest.
Arguments:
- tokens: bfloat16 [2048, 2048], P(('gr', 'tp')), may hold values from -6 to 6
- norm_gain: float32 [2048], P('fs'), may hold values from 0.1 to 1.9
- up_weight: float32 [2048, 8192], P('fs', ('gr', 'tp')), may hold values from -0.125 to 0.125
- down_weight: float32 [8192, 2048], P('fs', ('gr', 'tp')), may hold values from -0.09375 to 0.09375
Outputs:
- sampler_up: bfloat16 [2048, 8192], P(None, 'fs')
- sampler_down: bfloat16 [8192, 2048], P('fs')
- mixed: bfloat16 [2048, 2048], P(('gr', 'tp'), 'fs')
The draws below stay inside these ranges and needn't reach their ends.
All inputs are finite; a program needn't handle non-finite values.
Results may differ from the reference program's by a relative error of at most 0.023.
Values may be sent and summed in bfloat16 or wider, within the bound.
No kernel may reach another device: no remote copies, remote signals or barrier semaphores. Data moves between devices by JAX's collectives and lax.ppermute only.
A program may use at most 64 MiB of HBM per device.

```python
import jax
import jax.numpy as jnp
from jax import lax

D = 2048
FF = 8192
ROWS = 2048
N_FS = 8


def spiked(drawn, stream_key, source, target, blocks, factor):
    owner, partner = [(jnp.arange(drawn.shape[position]) // (drawn.shape[position] // blocks)).reshape([-1 if axis == position else 1 for axis in range(drawn.ndim)]) for position in (source, target)]
    chosen = jax.random.permutation(stream_key, blocks)[partner]
    strong = (owner == chosen) | (owner == (partner + blocks // 2) % blocks)
    return jnp.where(strong, factor * drawn, drawn)


def block_levels(rng, shape, cuts, smallest, top_value):
    gain, own = 1.0, jax.random.fold_in(rng, 6)
    for axis_at, blocks in cuts:
        draws = jnp.exp(jax.random.uniform(jax.random.fold_in(own, axis_at), (blocks,), jnp.float32, smallest / len(cuts), top_value / len(cuts)))
        gain = gain * jnp.repeat(draws, shape[axis_at] // blocks).reshape([-1 if axis == axis_at else 1 for axis in range(len(shape))])
    return gain


def bell_draw(key, extent, deviation, bound, cuts=(), held_as=jnp.bfloat16):
    result = jax.random.normal(key, extent, jnp.float32) * deviation
    if len(cuts) > 0:
        result = block_levels(key, extent, cuts, -0.22, 0.18) * result
    return jnp.clip(result, min=-bound, max=bound).astype(held_as)


def heavy_noise(own_key, dims, spread, limit, shards, heavy, held_as=jnp.bfloat16):
    entries = spread * jax.random.normal(own_key, dims, jnp.float32)
    if shards:
        entries = entries * block_levels(own_key, dims, shards, -0.22, 0.18)
    return jnp.clip(spiked(entries, jax.random.fold_in(own_key, 3), *heavy), -limit, limit).astype(held_as)


def setup_inputs(seed: int = 0) -> dict:
    streams_of = jax.random.split(jax.random.key(seed), 5)
    tokens = bell_draw(streams_of[0], (ROWS, D), 1.0, 6.0, ((0, 4),))
    norm_gain = jnp.clip(1.0 + 0.18 * jax.random.normal(streams_of[1], (D,), jnp.float32), 0.1, 1.9)
    up_weight = bell_draw(streams_of[2], (D, FF), D ** -0.5, 0.125, ((0, 8), (1, 4)), jnp.float32)
    down_weight = heavy_noise(streams_of[3], (FF, D), FF ** -0.5, 0.09375, ((0, 8), (1, 4)), (0, 1, 8, 2.0), jnp.float32)
    return dict(tokens=tokens, norm_gain=norm_gain, up_weight=up_weight, down_weight=down_weight)


def reference(tokens, norm_gain, up_weight, down_weight):
    sampler_up = (norm_gain[:, None] * up_weight).astype(jnp.bfloat16)
    sampler_down = down_weight.astype(jnp.bfloat16)
    widened = tokens.astype(jnp.float32)
    normed = (widened * lax.rsqrt(lax.optimization_barrier(jnp.mean(widened * widened, axis=-1, keepdims=True)) + 1e-06)).astype(jnp.bfloat16)
    preact = jnp.dot(normed, sampler_up, preferred_element_type=jnp.float32)
    hidden = jnp.square(jax.nn.relu(preact)).astype(jnp.bfloat16)
    block_units = FF // N_FS

    def add_block(total, index):
        begin = (index * block_units).astype(jnp.int32)
        hidden_part = lax.dynamic_slice_in_dim(hidden, begin, block_units, 1)
        down_part = lax.dynamic_slice_in_dim(sampler_down, begin, block_units, 0)
        partial_value = jnp.dot(hidden_part, down_part, preferred_element_type=jnp.float32).astype(jnp.bfloat16)
        partial_value = lax.optimization_barrier(partial_value)
        return (total + partial_value.astype(jnp.float32), None)
    start_total = jnp.zeros((tokens.shape[0], D), jnp.float32)
    summed, _ = lax.scan(add_block, start_total, jnp.arange(N_FS, dtype=jnp.int32))
    return (sampler_up, sampler_down, summed.astype(jnp.bfloat16))
```

```python
import jax
import jax.numpy as jnp
from jax import lax
from jax.sharding import PartitionSpec as P

AXES = ("gr", "fs", "tp")


def shifted(index, step, size):
    return index ^ step if size & (size - 1) == 0 else (index + step) % size


def unshifted(index, step, size):
    return index ^ step if size & (size - 1) == 0 else (index - step) % size


def per_device(sizes, tokens, norm_gain, up_weight, down_weight):
    planes, shards, cores = sizes
    parts = shards // (planes * cores)
    lines = planes * cores
    g, f, t = (lax.axis_index(name) for name in AXES)
    f_high, f_mid, f_low = f // (cores * parts), (f // parts) % cores, f % parts

    def send(value, target):
        pairs = []
        for sg in range(planes):
            for sf in range(shards):
                for st in range(cores):
                    to = target(sg, sf // (cores * parts), (sf // parts) % cores, sf % parts, st)
                    if to is not None:
                        tg, th, tm, tl, tt = to
                        tf = (th * cores + tm) * parts + tl
                        pairs.append(
                            ((sg * shards + sf) * cores + st, (tg * shards + tf) * cores + tt)
                        )
        return lax.ppermute(value, AXES, pairs)

    rows, columns = up_weight.shape
    units = columns // parts
    half = units // cores

    gain = norm_gain[:, None]
    received = []
    for b in range(parts):
        for c in range(cores):
            at = (shifted(f_low, b, parts) * cores + shifted(f_mid, c, cores)) * half
            own = (gain * lax.dynamic_slice(up_weight, (0, at), (rows, half))).astype(jnp.bfloat16)
            held = [own] + [
                send(own, lambda sg, h, m, l, st: (unshifted(sg, d, planes), h, m, l, st))
                for d in range(1, planes)
            ]
            for a in range(planes):

                def target(sg, h, m, l, st, d=None):
                    to = shifted(h, a, planes)
                    if d is not None and to != shifted(sg, d, planes):
                        return None
                    return (sg, to, st, shifted(l, b, parts), shifted(m, c, cores))

                if a == 0:
                    which = held[0]
                    for d in range(1, planes):
                        which = jnp.where(f_high == shifted(g, d, planes), held[d], which)
                    got = send(which, target)
                else:
                    got = None
                    for d in range(planes):
                        one = send(held[d], lambda *s: target(*s, d=d))
                        got = one if got is None else jnp.where(f_high == shifted(g, d, planes), one, got)
                received.append((a, b, c, got))
    up_block = jnp.zeros((shards * rows, units), jnp.bfloat16)
    for step in range(cores):
        for a, b, c, got in received:
            core = shifted(t, step, cores)
            piece = got
            if step:
                piece = send(got, lambda sg, h, m, l, st: (sg, h, m, l, unshifted(st, step, cores)))
            source = (
                (unshifted(f_high, a, planes) * cores + unshifted(core, c, cores)) * parts
                + unshifted(f_low, b, parts)
            )
            up_block = lax.dynamic_update_slice(up_block, piece, (source * rows, core * half))

    down_own = down_weight.astype(jnp.bfloat16)
    width = down_own.shape[1]
    down_columns = jnp.zeros((down_own.shape[0], width * lines), jnp.bfloat16)
    for d in range(planes):
        crossed = down_own
        if d:
            crossed = send(down_own, lambda sg, h, m, l, st: (unshifted(sg, d, planes), h, m, l, st))
        for step in range(cores):
            piece = crossed
            if step:
                piece = send(crossed, lambda sg, h, m, l, st: (sg, h, m, l, unshifted(st, step, cores)))
            at = (shifted(g, d, planes) * cores + shifted(t, step, cores)) * width
            down_columns = lax.dynamic_update_slice(down_columns, piece, (0, at))

    widened = tokens.astype(jnp.float32)
    normed = (
        widened * lax.rsqrt(jnp.mean(widened * widened, axis=-1, keepdims=True) + 1e-06)
    ).astype(jnp.bfloat16)
    preact = jnp.dot(normed, up_block, preferred_element_type=jnp.float32)
    hidden = jnp.square(jax.nn.relu(preact)).astype(jnp.bfloat16)

    narrow = width // parts
    line = f // parts
    total = None
    for s in reversed(range(lines)):
        to_line = shifted(line, s, lines)
        block = lax.dynamic_slice(down_columns, (0, to_line * width), (down_own.shape[0], width))
        partial = jnp.dot(hidden, block, preferred_element_type=jnp.float32).astype(jnp.bfloat16)

        def cut(low):
            return lax.dynamic_slice(partial, (0, low * narrow), (partial.shape[0], narrow))

        summed = cut(f_low).astype(jnp.float32)
        for b in range(1, parts):
            got = send(
                cut(shifted(f_low, b, parts)),
                lambda sg, h, m, l, st: (sg, h, m, shifted(l, b, parts), st),
            )
            summed = summed + got.astype(jnp.float32)
        if s:

            def along(sg, h, m, l, st):
                to = shifted(h * cores + m, s, lines)
                return (sg, to // cores, to % cores, l, st)

            summed = send(summed.astype(jnp.bfloat16), along).astype(jnp.float32)
        total = summed if total is None else total + summed
    return (up_block, down_columns, total.astype(jnp.bfloat16))


def solution(mesh):
    sizes = tuple(mesh.shape[name] for name in AXES)
    in_specs = (P(("gr", "tp"), None), P("fs"), P("fs", ("gr", "tp")), P("fs", ("gr", "tp")))
    out_specs = (P(None, "fs"), P("fs", None), P(("gr", "tp"), "fs"))
    return jax.shard_map(
        lambda *args: per_device(sizes, *args),
        mesh=mesh,
        in_specs=in_specs,
        out_specs=out_specs,
        check_vma=False,
    )
```

```python
import jax
import jax.numpy as jnp
from jax import lax
from jax.sharding import PartitionSpec as P

AXES = ("gr", "fs", "tp")
BOTH = {(1, 0): True, (1, 1): False, (0, 0): False, (0, 1): False}


def per_device(sizes, tokens, norm_gain, up_weight, down_weight):
    planes, shards, cores = sizes
    parts = shards // (planes * cores)
    lines = planes * cores
    g, f, t = (lax.axis_index(name) for name in AXES)
    f_high, f_mid, f_low = f // (cores * parts), (f // parts) % cores, f % parts

    def send(value, target):
        pairs = []
        for sg in range(planes):
            for sf in range(shards):
                for st in range(cores):
                    to = target(sg, sf // (cores * parts), (sf // parts) % cores, sf % parts, st)
                    if to is not None:
                        tg, th, tm, tl, tt = to
                        tf = (th * cores + tm) * parts + tl
                        pairs.append(
                            ((sg * shards + sf) * cores + st, (tg * shards + tf) * cores + tt)
                        )
        return lax.ppermute(value, AXES, pairs)

    rows, columns = up_weight.shape
    units = columns // parts
    share = rows // planes

    def own_piece(b, h):
        at = (f_low ^ b) * units
        weight = lax.dynamic_slice(up_weight, (h * share, at), (share, units))
        gain = lax.dynamic_slice(norm_gain, (h * share,), (share,))[:, None]
        return (gain * weight).astype(jnp.bfloat16)

    pieces = {}
    own = {(b, h): own_piece(b, h) for b in range(parts) for h in range(planes)}
    order = sorted(((a, b) for a in range(planes) for b in range(parts)), reverse=True)
    order = [(a, b) for a in reversed(range(planes)) for b in range(parts)]
    both = {(a, b): BOTH.get((a, b), False) for a, b in order}
    crossed = {}
    for b in range(parts):
        for d in range(1, planes):
            for h in reversed(range(planes)):
                if h == d:
                    crossed[b, d, h] = send(own[b, h], lambda sg, *r: (sg ^ d, *r))
                elif any(both[a, b] for a in range(planes)):

                    def wanted(sg, sh, m, l, st):
                        return (sg ^ d, sh, m, l, st) if both[sh ^ sg, b] else None

                    crossed[b, d, h] = send(own[b, h], wanted)
    for a, b in order:

        def target(sg, sh, m, l, st):
            return (sg, sh ^ a, st, l ^ b, m)

        plane = f_high ^ a
        for h in range(planes) if both[a, b] else (None,):
            value = own[b, 0 if h is None else h]
            for d in range(1, planes):
                value = jnp.where(plane == g ^ d, crossed[b, d, d if h is None else h], value)
            got = send(value, target)
            if h is not None:
                pieces[a, b, h] = [(got, h)]
            else:
                pieces[a, b, 0] = [(got, g ^ f_high)]
                for d in range(1, planes):
                    pieces[a, b, d] = [(send(got, lambda sg, *r: (sg ^ d, *r)), g ^ d ^ f_high)]
    up_block = jnp.zeros((shards * planes, share, units), jnp.bfloat16)
    for (a, b, _), [(got, h)] in pieces.items():
        for step in range(cores):
            piece, where = got, h
            if step:
                piece = send(got, lambda sg, sh, m, l, st: (sg, sh, m, l, st ^ step))
            source = ((f_high ^ a) * cores + (t ^ step)) * parts + (f_low ^ b)
            up_block = lax.dynamic_update_slice(
                up_block, piece[None], (source * planes + where, 0, 0)
            )
    up_block = up_block.reshape(shards * rows, units)

    down_own = down_weight.astype(jnp.bfloat16)
    width = down_own.shape[1]
    down_columns = jnp.zeros((down_own.shape[0], width * lines), jnp.bfloat16)
    for d in range(planes):
        piece = send(down_own, lambda sg, *r: (sg ^ d, *r)) if d else down_own
        for step in range(cores):
            swapped = piece
            if step:
                swapped = send(piece, lambda sg, sh, m, l, st: (sg, sh, m, l, st ^ step))
            at = ((g ^ d) * cores + (t ^ step)) * width
            down_columns = lax.dynamic_update_slice(down_columns, swapped, (0, at))

    widened = tokens.astype(jnp.float32)
    normed = (
        widened * lax.rsqrt(jnp.mean(widened * widened, axis=-1, keepdims=True) + 1e-06)
    ).astype(jnp.bfloat16)
    preact = jnp.dot(normed, up_block, preferred_element_type=jnp.float32)
    hidden = jnp.square(jax.nn.relu(preact)).astype(jnp.bfloat16)

    narrow = width // parts
    line = f // parts
    total = None
    for s in reversed(range(lines)):
        block = lax.dynamic_slice(down_columns, (0, (line ^ s) * width), (down_own.shape[0], width))
        partial = jnp.dot(hidden, block, preferred_element_type=jnp.float32).astype(jnp.bfloat16)

        def cut(low):
            return lax.dynamic_slice(partial, (0, low * narrow), (partial.shape[0], narrow))

        summed = cut(f_low).astype(jnp.float32)
        for b in range(1, parts):
            got = send(cut(f_low ^ b), lambda sg, sh, m, l, st: (sg, sh, m, l ^ b, st))
            summed = summed + got.astype(jnp.float32)
        if s:

            def along(sg, sh, m, l, st):
                to = (sh * cores + m) ^ s
                return (sg, to // cores, to % cores, l, st)

            summed = send(summed.astype(jnp.bfloat16), along).astype(jnp.float32)
        total = summed if total is None else total + summed
    return (up_block, down_columns, total.astype(jnp.bfloat16))


def solution(mesh):
    sizes = tuple(mesh.shape[name] for name in AXES)
    in_specs = (P(("gr", "tp"), None), P("fs"), P("fs", ("gr", "tp")), P("fs", ("gr", "tp")))
    out_specs = (P(None, "fs"), P("fs", None), P(("gr", "tp"), "fs"))
    return jax.shard_map(
        lambda *args: per_device(sizes, *args),
        mesh=mesh,
        in_specs=in_specs,
        out_specs=out_specs,
        check_vma=False,
    )
```

```python
import functools

import jax
import jax.numpy as jnp
from jax import lax
from jax.experimental import pallas as pl
from jax.experimental.pallas import tpu as pltpu
from jax.sharding import PartitionSpec as P

AXES = ("gr", "fs", "tp")
BOTH = {(1, 0): False, (1, 1): False, (0, 0): False, (0, 1): False}


def layer_kernel(counts, slots, normed, *refs):
    n_up, n_down, n_out = counts
    ups, downs, refs = refs[:n_up], refs[n_up : n_up + n_down], refs[n_up + n_down :]
    up_out, down_out, outs, refs = refs[0], refs[1], refs[2 : 2 + n_out], refs[2 + n_out :]
    tokens_v, up_v, down_v, hidden_v, in_sem, out_sem = refs
    share, width, narrow = ups[0].shape[0], downs[0].shape[1], outs[0].shape[1]

    loads = [pltpu.make_async_copy(normed, tokens_v, in_sem.at[0])]
    for i, piece in enumerate(ups):
        at = pl.multiple_of(slots[i] * share, share)
        loads.append(pltpu.make_async_copy(piece, up_v.at[pl.ds(at, share)], in_sem.at[1 + i]))
    for i, piece in enumerate(downs):
        at = pl.multiple_of(slots[n_up + i] * width, width)
        loads.append(
            pltpu.make_async_copy(piece, down_v.at[:, pl.ds(at, width)], in_sem.at[1 + n_up + i])
        )
    for load in loads:
        load.start()
    for load in loads[: 1 + n_up]:
        load.wait()
    up_store = pltpu.make_async_copy(up_v, up_out, out_sem.at[0])
    up_store.start()
    tile = min(256, up_v.shape[1])

    @pl.loop(0, up_v.shape[1] // tile)
    def _(i):
        cols = pl.ds(pl.multiple_of(i * tile, tile), tile)
        preact = jnp.dot(tokens_v[...], up_v[:, cols], preferred_element_type=jnp.float32)
        hidden_v[:, cols] = jnp.square(jax.nn.relu(preact)).astype(jnp.bfloat16)

    for load in loads[1 + n_up :]:
        load.wait()
    down_store = pltpu.make_async_copy(down_v, down_out, out_sem.at[1])
    down_store.start()
    for i, out in enumerate(outs):
        cols = pl.ds(pl.multiple_of(slots[n_up + n_down + i] * narrow, narrow), narrow)
        out[...] = jnp.dot(
            hidden_v[...], down_v[:, cols], preferred_element_type=jnp.float32
        ).astype(jnp.bfloat16)
    up_store.wait()
    down_store.wait()


def layer(normed, ups, up_slots, downs, down_slots, out_slots):
    share, units = ups[0].shape
    depth, width = downs[0].shape
    narrow = width * len(downs) // len(out_slots)
    slots = jnp.stack([jnp.int32(s) for s in (*up_slots, *down_slots, *out_slots)])
    counts = (len(ups), len(downs), len(out_slots))
    count = normed.shape[0]
    any_space, vmem = pl.BlockSpec(memory_space=pl.ANY), pl.BlockSpec(memory_space=pltpu.VMEM)
    bf16 = jnp.bfloat16
    up_shape, down_shape = (share * len(ups), units), (depth, width * len(downs))
    flops = 2 * count * (up_shape[0] * units + depth * down_shape[1])
    up_block, down_columns, *outs = pl.pallas_call(
        functools.partial(layer_kernel, counts),
        out_shape=[
            jax.ShapeDtypeStruct(up_shape, bf16),
            jax.ShapeDtypeStruct(down_shape, bf16),
            *[jax.ShapeDtypeStruct((count, narrow), bf16)] * len(out_slots),
        ],
        in_specs=[pl.BlockSpec(memory_space=pltpu.SMEM)] + [any_space] * (1 + sum(counts[:2])),
        out_specs=[any_space] * 2 + [vmem] * len(out_slots),
        scratch_shapes=[
            pltpu.VMEM(normed.shape, bf16),
            pltpu.VMEM(up_shape, bf16),
            pltpu.VMEM(down_shape, bf16),
            pltpu.VMEM((count, units), bf16),
            pltpu.SemaphoreType.DMA((1 + sum(counts[:2]),)),
            pltpu.SemaphoreType.DMA((2,)),
        ],
        compiler_params=pltpu.CompilerParams(vmem_limit_bytes=32 << 20),
        cost_estimate=pl.CostEstimate(flops=flops, bytes_accessed=20 << 20, transcendentals=0),
    )(slots, normed, *ups, *downs)
    return up_block, down_columns, outs


def per_device(sizes, tokens, norm_gain, up_weight, down_weight):
    planes, shards, cores = sizes
    parts = shards // (planes * cores)
    lines = planes * cores
    g, f, t = (lax.axis_index(name) for name in AXES)
    f_high, f_mid, f_low = f // (cores * parts), (f // parts) % cores, f % parts

    def send(value, target):
        pairs = []
        for sg in range(planes):
            for sf in range(shards):
                for st in range(cores):
                    to = target(sg, sf // (cores * parts), (sf // parts) % cores, sf % parts, st)
                    if to is not None:
                        tg, th, tm, tl, tt = to
                        tf = (th * cores + tm) * parts + tl
                        pairs.append(
                            ((sg * shards + sf) * cores + st, (tg * shards + tf) * cores + tt)
                        )
        return lax.ppermute(value, AXES, pairs)

    rows, columns = up_weight.shape
    units = columns // parts
    share = rows // planes

    def own_piece(b, h):
        at = (f_low ^ b) * units
        weight = lax.dynamic_slice(up_weight, (h * share, at), (share, units))
        gain = lax.dynamic_slice(norm_gain, (h * share,), (share,))[:, None]
        return (gain * weight).astype(jnp.bfloat16)

    pieces = {}
    own = {(b, h): own_piece(b, h) for b in range(parts) for h in range(planes)}
    order = sorted(((a, b) for a in range(planes) for b in range(parts)), reverse=True)
    order = [(a, b) for a in reversed(range(planes)) for b in range(parts)]
    both = {(a, b): BOTH.get((a, b), False) for a, b in order}
    crossed = {}
    for b in range(parts):
        for d in range(1, planes):
            for h in reversed(range(planes)):
                if h == d:
                    crossed[b, d, h] = send(own[b, h], lambda sg, *r: (sg ^ d, *r))
                elif any(both[a, b] for a in range(planes)):

                    def wanted(sg, sh, m, l, st):
                        return (sg ^ d, sh, m, l, st) if both[sh ^ sg, b] else None

                    crossed[b, d, h] = send(own[b, h], wanted)
    for a, b in order:

        def target(sg, sh, m, l, st):
            return (sg, sh ^ a, st, l ^ b, m)

        plane = f_high ^ a
        for h in range(planes) if both[a, b] else (None,):
            value = own[b, 0 if h is None else h]
            for d in range(1, planes):
                value = jnp.where(plane == g ^ d, crossed[b, d, d if h is None else h], value)
            got = send(value, target)
            if h is not None:
                pieces[a, b, h] = [(got, h)]
            else:
                pieces[a, b, 0] = [(got, g ^ f_high)]
                for d in range(1, planes):
                    pieces[a, b, d] = [(send(got, lambda sg, *r: (sg ^ d, *r)), g ^ d ^ f_high)]
    ups, up_slots = [], []
    for (a, b, _), [(got, h)] in pieces.items():
        for step in range(cores):
            piece = got
            if step:
                piece = send(got, lambda sg, sh, m, l, st: (sg, sh, m, l, st ^ step))
            source = ((f_high ^ a) * cores + (t ^ step)) * parts + (f_low ^ b)
            ups.append(piece)
            up_slots.append(source * planes + h)

    down_own, _ = lax.optimization_barrier((down_weight, list(crossed.values())))
    down_own = down_own.astype(jnp.bfloat16)
    width = down_own.shape[1]
    downs, down_slots = [], []
    for d in range(planes):
        piece = send(down_own, lambda sg, *r: (sg ^ d, *r)) if d else down_own
        for step in range(cores):
            swapped = piece
            if step:
                swapped = send(piece, lambda sg, sh, m, l, st: (sg, sh, m, l, st ^ step))
            downs.append(swapped)
            down_slots.append((g ^ d) * cores + (t ^ step))

    widened = tokens.astype(jnp.float32)
    normed = (
        widened * lax.rsqrt(jnp.mean(widened * widened, axis=-1, keepdims=True) + 1e-06)
    ).astype(jnp.bfloat16)
    narrow = width // parts
    line = f // parts
    order = [(s, b) for s in reversed(range(lines)) for b in reversed(range(parts))]
    out_slots = [(line ^ s) * parts + (f_low ^ b) for s, b in order]
    if narrow % 128 == 0 and share % 16 == 0:
        up_block, down_columns, outs = layer(normed, ups, up_slots, downs, down_slots, out_slots)
    else:
        up_block = jnp.zeros((len(ups), share, units), jnp.bfloat16)
        for piece, slot in zip(ups, up_slots):
            up_block = lax.dynamic_update_slice(up_block, piece[None], (slot, 0, 0))
        up_block = up_block.reshape(shards * rows, units)
        down_columns = jnp.zeros((down_own.shape[0], width * lines), jnp.bfloat16)
        for piece, slot in zip(downs, down_slots):
            down_columns = lax.dynamic_update_slice(down_columns, piece, (0, slot * width))
        preact = jnp.dot(normed, up_block, preferred_element_type=jnp.float32)
        hidden = jnp.square(jax.nn.relu(preact)).astype(jnp.bfloat16)
        outs = []
        for slot in out_slots:
            block = lax.dynamic_slice(down_columns, (0, slot * narrow), (units, narrow))
            outs.append(jnp.dot(hidden, block, preferred_element_type=jnp.float32).astype(jnp.bfloat16))
    partial = dict(zip(order, outs))

    total = None
    for s in reversed(range(lines)):
        summed = partial[s, 0].astype(jnp.float32)
        for b in range(1, parts):
            got = send(partial[s, b], lambda sg, sh, m, l, st: (sg, sh, m, l ^ b, st))
            summed = summed + got.astype(jnp.float32)
        if s:

            def along(sg, sh, m, l, st):
                to = (sh * cores + m) ^ s
                return (sg, to // cores, to % cores, l, st)

            summed = send(summed.astype(jnp.bfloat16), along).astype(jnp.float32)
        total = summed if total is None else total + summed
    return (up_block, down_columns, total.astype(jnp.bfloat16))


def solution(mesh):
    sizes = tuple(mesh.shape[name] for name in AXES)
    in_specs = (P(("gr", "tp"), None), P("fs"), P("fs", ("gr", "tp")), P("fs", ("gr", "tp")))
    out_specs = (P(None, "fs"), P("fs", None), P(("gr", "tp"), "fs"))
    return jax.shard_map(
        lambda *args: per_device(sizes, *args),
        mesh=mesh,
        in_specs=in_specs,
        out_specs=out_specs,
        check_vma=False,
    )
```
